32 devices in a mesh: grp: 2 (over y), fs: 4 (over z), tp: 4 (over x, core).
Axes of the slice: x: 2, y: 2, z: 4, core: 2. Of those that a mesh axis runs over, the one named last changes fastest.
Arguments:
- tokens: bfloat16 [2048, 2048], P(('grp', 'fs')), parts along dimension 0, may hold values from -6 to 6
- ffn_pre_gain: bfloat16 [2048], replicated, may hold values from 0.099609375 to 1.8984375
- gate_weight: bfloat16 [2048, 5632], P('fs', 'tp'), may hold values from -0.125 to 0.125
- up_weight: bfloat16 [2048, 5632], P('fs', 'tp'), may hold values from -0.125 to 0.125
- down_weight: bfloat16 [5632, 2048], P('tp', 'fs'), may hold values from -0.078125 to 0.078125
- ffn_post_gain: bfloat16 [2048], replicated, may hold values from 0.099609375 to 1.8984375
- mix_pre_gain: bfloat16 [2048], replicated, may hold values from 0.099609375 to 1.8984375
- mix_u_weight: bfloat16 [2048, 2048], P('fs', 'tp'), may hold values from -0.125 to 0.125
- mix_v_weight: bfloat16 [2048, 2048], P('fs', 'tp'), may hold values from -0.125 to 0.125
- spatial_gain: bfloat16 [2048], P('tp'), may hold values from 0.099609375 to 1.8984375
- spatial_weight: bfloat16 [16, 128, 128], P('tp'), may hold values from -0.5 to 0.5
- spatial_bias: bfloat16 [16, 128], P('tp'), may hold values from 0.099609375 to 1.8984375
- mix_out_weight: bfloat16 [2048, 2048], P('tp', 'fs'), may hold values from -0.125 to 0.125
- mix_post_gain: bfloat16 [2048], replicated, may hold values from 0.099609375 to 1.8984375
- late_pre_gain: bfloat16 [2048], replicated, may hold values from 0.099609375 to 1.8984375
- late_post_gain: bfloat16 [2048], replicated, may hold values from 0.099609375 to 1.8984375
Outputs:
- result: bfloat16 [2048, 2048], P(('grp', 'fs')), parts along dimension 0
The draws below stay inside these ranges and needn't reach their ends.
There are 2 independent parts, one for each index of `grp`. The reference program is written for one: setup_inputs(seed, part) draws one part's arguments, and reference() takes and returns one part's arrays. A program takes and returns all parts, laid end to end along the dimension named above; an argument that names none is the same for every part. Nothing has to cross between parts.
All inputs are finite; a program needn't handle non-finite values.
Results may differ from the reference program's by a relative error of at most 0.019.
Values may be sent and summed in bfloat16 or wider, within the bound.
A program may use at most 128 MiB of HBM per device.

```python
import jax
import jax.numpy as jnp
from jax import lax

D = 2048
FF = 5632
MIX_WIDTH = 2048
GROUP_WIDTH = 128
BLOCK = 128
GROUPS = 16
TOKENS = 1024
N_TP = 4


def block_scale(stream_key, extent, split, smallest, top_value):
    def one(dim, shards_of):
        steps = jax.random.uniform(jax.random.fold_in(jax.random.fold_in(stream_key, 6), dim), (shards_of,), jnp.float32, smallest / len(split), top_value / len(split))
        return jnp.repeat(jnp.exp(steps), extent[dim] // shards_of).reshape((-1,) + (1,) * (len(extent) - dim - 1))

    loudness = one(*split[0])
    for cut in split[1:]:
        loudness = loudness * one(*cut)
    return loudness


def noise(own_key, dims, scale, reach, cuts=(), kind=jnp.bfloat16):
    entries = jax.random.normal(own_key, dims, jnp.float32) * scale
    if len(cuts) > 0:
        entries = block_scale(own_key, dims, cuts, -0.22, 0.18) * entries
    return jnp.clip(entries, min=-reach, max=reach).astype(kind)


def setup_inputs(seed: int = 0, part: int = 0) -> dict:
    seeds = jax.random.split(jax.random.key(seed), 17)
    own_keys = jax.random.split(jax.random.fold_in(seeds[16], part), 17)
    return {
        "tokens": noise(own_keys[0], (TOKENS, D), 1.0, 6.0, ((0, 4),)),
        "ffn_pre_gain": jnp.clip(1.0 + 0.18 * jax.random.normal(seeds[1], (D,), jnp.float32), 0.099609375, 1.8984375).astype(jnp.bfloat16),
        "gate_weight": noise(seeds[2], (D, FF), D ** -0.5, 0.125, ((0, 4), (1, 4))),
        "up_weight": noise(seeds[3], (D, FF), D ** -0.5, 0.125, ((0, 4), (1, 4))),
        "down_weight": noise(seeds[4], (FF, D), FF ** -0.5, 0.078125, ((0, 4), (1, 4))),
        "ffn_post_gain": jnp.clip(1.0 + 0.18 * jax.random.normal(seeds[5], (D,), jnp.float32), 0.099609375, 1.8984375).astype(jnp.bfloat16),
        "mix_pre_gain": jnp.clip(1.0 + 0.18 * jax.random.normal(seeds[6], (D,), jnp.float32), 0.099609375, 1.8984375).astype(jnp.bfloat16),
        "mix_u_weight": noise(seeds[7], (D, MIX_WIDTH), D ** -0.5, 0.125, ((0, 4), (1, 4))),
        "mix_v_weight": noise(seeds[8], (D, MIX_WIDTH), D ** -0.5, 0.125, ((0, 4), (1, 4))),
        "spatial_gain": jnp.clip(1.0 + 0.18 * jax.random.normal(seeds[9], (MIX_WIDTH,), jnp.float32), 0.099609375, 1.8984375).astype(jnp.bfloat16),
        "spatial_weight": noise(seeds[10], (GROUPS, BLOCK, BLOCK), BLOCK ** -0.5, 0.5, ((0, 4),)),
        "spatial_bias": jnp.clip(1.0 + 0.18 * jax.random.normal(seeds[11], (GROUPS, BLOCK), jnp.float32), 0.099609375, 1.8984375).astype(jnp.bfloat16),
        "mix_out_weight": noise(seeds[12], (MIX_WIDTH, D), MIX_WIDTH ** -0.5, 0.125, ((0, 4), (1, 4))),
        "mix_post_gain": jnp.clip(1.0 + 0.18 * jax.random.normal(seeds[13], (D,), jnp.float32), 0.099609375, 1.8984375).astype(jnp.bfloat16),
        "late_pre_gain": jnp.clip(1.0 + 0.18 * jax.random.normal(seeds[14], (D,), jnp.float32), 0.099609375, 1.8984375).astype(jnp.bfloat16),
        "late_post_gain": jnp.clip(1.0 + 0.18 * jax.random.normal(seeds[15], (D,), jnp.float32), 0.099609375, 1.8984375).astype(jnp.bfloat16),
    }


def row_norm(values, gain):
    scale = lax.rsqrt(lax.optimization_barrier(jnp.mean(values * values, axis=-1, keepdims=True)) + 1e-06)
    return values * scale * gain.astype(jnp.float32)

def split_sum(left, right, pieces):
    width = left.shape[1] // pieces
    total = jnp.zeros((left.shape[0], right.shape[1]), jnp.float32)
    for index in range(pieces):
        partial_term = jnp.dot(left[:, index * width:(index + 1) * width], right[index * width:(index + 1) * width], preferred_element_type=jnp.float32)
        rounded = lax.optimization_barrier(partial_term.astype(jnp.bfloat16))
        total = total + rounded.astype(jnp.float32)
    return total

def feed_forward(stream, pre_gain, post_gain, gate_weight, up_weight, down_weight):
    normed = row_norm(stream.astype(jnp.float32), pre_gain).astype(jnp.bfloat16)
    gate = jnp.dot(normed, gate_weight, preferred_element_type=jnp.float32)
    upper = jnp.dot(normed, up_weight, preferred_element_type=jnp.float32)
    hidden = (jax.nn.silu(gate) * upper).astype(jnp.bfloat16)
    branch = split_sum(hidden, down_weight, N_TP)
    return (stream.astype(jnp.float32) + 0.5 * row_norm(branch, post_gain)).astype(jnp.bfloat16)

def reference(tokens, ffn_pre_gain, gate_weight, up_weight, down_weight, ffn_post_gain, mix_pre_gain, mix_u_weight, mix_v_weight, spatial_gain, spatial_weight, spatial_bias, mix_out_weight, mix_post_gain, late_pre_gain, late_post_gain):
    first = feed_forward(tokens, ffn_pre_gain, ffn_post_gain, gate_weight, up_weight, down_weight)
    normed = row_norm(first.astype(jnp.float32), mix_pre_gain).astype(jnp.bfloat16)
    gated_u = jax.nn.gelu(jnp.dot(normed, mix_u_weight, preferred_element_type=jnp.float32), approximate=False)
    gating_v = jax.nn.gelu(jnp.dot(normed, mix_v_weight, preferred_element_type=jnp.float32), approximate=False)
    count = gating_v.shape[0]
    grouped = gating_v.reshape(count, GROUPS, GROUP_WIDTH)
    centred = grouped - lax.optimization_barrier(jnp.mean(grouped, axis=-1, keepdims=True))
    vnorm = centred * lax.rsqrt(lax.optimization_barrier(jnp.mean(centred * centred, axis=-1, keepdims=True)) + 1e-05)
    vnorm = (vnorm * spatial_gain.astype(jnp.float32).reshape(GROUPS, GROUP_WIDTH)).astype(jnp.bfloat16)
    blocks = vnorm.reshape(count // BLOCK, BLOCK, GROUPS, GROUP_WIDTH).astype(jnp.float32)
    lower = jnp.tril(jnp.ones((BLOCK, BLOCK), dtype=bool))
    masked = jnp.where(lower[None], spatial_weight, jnp.zeros_like(spatial_weight)).astype(jnp.float32)
    spatial = jnp.einsum('gts,nsgc->ntgc', masked, blocks)
    spatial = spatial + spatial_bias.astype(jnp.float32).T[None, :, :, None]
    mixed = (gated_u * spatial.reshape(count, MIX_WIDTH)).astype(jnp.bfloat16)
    branch = split_sum(mixed, mix_out_weight, N_TP)
    second = (first.astype(jnp.float32) + row_norm(branch, mix_post_gain)).astype(jnp.bfloat16)
    return feed_forward(second, late_pre_gain, late_post_gain, gate_weight, up_weight, down_weight)
```

```python
import functools

import jax
import jax.numpy as jnp
from jax import lax
from jax.experimental import pallas as pl
from jax.experimental.pallas import tpu as pltpu
from jax.sharding import PartitionSpec as P

GROUP_WIDTH = 128
BLOCK = 128
TILE = 256
F32 = jnp.float32
BF16 = jnp.bfloat16
MESH = pl.DeviceIdType.MESH
SPLITS = (2, 2, 2, 1, 1, 1)


def aligned(value, unit):
    return value if isinstance(value, int) else pl.multiple_of(value, unit)


def over_tiles(width, body):
    count = width // TILE

    def step(i, carry):
        body(pl.multiple_of(i * TILE, TILE), TILE)
        return carry

    lax.fori_loop(0, count, step, 0)
    if width % TILE:
        body(count * TILE, width % TILE)


def over_rows(count, size, body):
    def step(i, carry):
        body(pl.multiple_of(i * size, size))
        return carry

    lax.fori_loop(0, count // size, step, 0)


def gelu(a):
    return 0.5 * a * (1.0 + lax.erf(a * (2.0**-0.5)))


def kernel(
    sizes,
    tokens,
    gains,
    gate_w,
    up_w,
    down_w,
    u_w,
    v_w,
    out_w,
    spatial_gain,
    spatial_weight,
    spatial_bias,
    result,
    gate_full,
    up_full,
    down_full,
    u_full,
    v_full,
    out_full,
    normed,
    hidden,
    mixed,
    parts,
    landed,
    streams,
    own_sem,
    left_send,
    left_recv,
    right_send,
    right_recv,
    side_send,
    side_recv,
    sum_send,
    sum_recv,
    put_send,
    put_recv,
    last_sem,
):
    grp_n, fs_n, tp_n = sizes
    grp, fs, tp = lax.axis_index("grp"), lax.axis_index("fs"), lax.axis_index("tp")
    shards = (gate_w, up_w, down_w, u_w, v_w, out_w)
    fulls = (gate_full, up_full, down_full, u_full, v_full, out_full)
    count, width = tokens.shape
    chunk = count // tp_n

    barrier = pltpu.get_barrier_semaphore()
    for move in (1, fs_n - 1):
        pl.semaphore_signal(
            barrier, inc=1, device_id={"fs": lax.rem(fs + move, fs_n)}, device_id_type=MESH
        )
    for move in range(1, grp_n):
        pl.semaphore_signal(
            barrier, inc=1, device_id={"grp": lax.rem(grp + move, grp_n)}, device_id_type=MESH
        )
    for move in range(1, tp_n):
        pl.semaphore_signal(
            barrier, inc=1, device_id={"tp": lax.rem(tp + move, tp_n)}, device_id_type=MESH
        )
    pl.semaphore_wait(barrier, 2 + grp_n - 1 + tp_n - 1)

    units = []
    for w in range(6):
        piece = shards[w].shape[0] // grp_n // SPLITS[w]
        for s in range(SPLITS[w]):
            units.append((w, s * piece, piece))

    def unit_rows(unit):
        w, low, piece = units[unit]
        return aligned(grp * (shards[w].shape[0] // grp_n) + low, 16), piece

    def place(w, block, low, piece):
        if w in (2, 5):
            return fulls[w].at[block, pl.ds(low, piece), :]
        start = aligned(block * shards[w].shape[0] + low, 16)
        return fulls[w].at[pl.ds(start, piece), :]

    def own_copy(w):
        return pltpu.make_async_copy(
            shards[w], place(w, fs, 0, shards[w].shape[0]), own_sem.at[w]
        )

    def to_right(unit, hop, own=False):
        w = units[unit][0]
        low, piece = unit_rows(unit)
        target = place(w, fs - hop, low, piece)
        source = shards[w].at[pl.ds(low, piece), :] if own else target
        return pltpu.make_async_remote_copy(
            src_ref=source,
            dst_ref=target,
            send_sem=right_send.at[unit, hop],
            recv_sem=right_recv.at[unit, hop],
            device_id={"fs": fs + 1},
            device_id_type=MESH,
        )

    def to_left(unit, hop, own=False):
        w = units[unit][0]
        low, piece = unit_rows(unit)
        target = place(w, fs + hop, low, piece)
        source = shards[w].at[pl.ds(low, piece), :] if own else target
        return pltpu.make_async_remote_copy(
            src_ref=source,
            dst_ref=target,
            send_sem=left_send.at[unit, hop],
            recv_sem=left_recv.at[unit, hop],
            device_id={"fs": fs - 1},
            device_id_type=MESH,
        )

    def to_side(unit, side, hop, move):
        w = units[unit][0]
        low, piece = unit_rows(unit)
        block = fs - hop if side == 0 else fs + hop
        target = place(w, block, low, piece)
        return pltpu.make_async_remote_copy(
            src_ref=target,
            dst_ref=target,
            send_sem=side_send.at[unit, side, move - 1, hop],
            recv_sem=side_recv.at[unit, side, move - 1, hop],
            device_id={"grp": lax.rem(grp + move, grp_n)},
            device_id_type=MESH,
        )

    def send_own(unit):
        if unit >= len(units):
            return

        @pl.when(fs < fs_n - 1)
        def _():
            to_right(unit, 0, own=True).start()

        @pl.when(fs > 0)
        def _():
            to_left(unit, 0, own=True).start()

    def relay(unit):
        def step(hop, carry):
            @pl.when(fs >= hop)
            def _():
                to_right(unit, hop - 1).wait_recv()

                @pl.when(fs < fs_n - 1)
                def _():
                    to_right(unit, hop).start()

                for move in range(1, grp_n):
                    to_side(unit, 0, hop, move).start()

            @pl.when(fs + hop < fs_n)
            def _():
                to_left(unit, hop - 1).wait_recv()

                @pl.when(fs > 0)
                def _():
                    to_left(unit, hop).start()

                for move in range(1, grp_n):
                    to_side(unit, 1, hop, move).start()

            return carry

        lax.fori_loop(1, fs_n, step, 0)

    def wait_weight(w):
        own_copy(w).wait()
        for unit in range(len(units)):
            if units[unit][0] == w:

                def step(hop, carry, unit=unit):
                    for move in range(1, grp_n):

                        @pl.when(fs >= hop)
                        def _():
                            to_side(unit, 0, hop, move).wait_recv()

                        @pl.when(fs + hop < fs_n)
                        def _():
                            to_side(unit, 1, hop, move).wait_recv()

                    return carry

                lax.fori_loop(1, fs_n, step, 0)

    def finish_sends():
        for unit in range(len(units)):

            def step(hop, carry, unit=unit):
                @pl.when((fs >= hop) & (fs < fs_n - 1))
                def _():
                    to_right(unit, hop).wait_send()

                @pl.when((fs + hop < fs_n) & (fs > 0))
                def _():
                    to_left(unit, hop).wait_send()

                @pl.when(hop > 0)
                def _():
                    for move in range(1, grp_n):

                        @pl.when(fs >= hop)
                        def _():
                            to_side(unit, 0, hop, move).wait_send()

                        @pl.when(fs + hop < fs_n)
                        def _():
                            to_side(unit, 1, hop, move).wait_send()

                return carry

            lax.fori_loop(0, fs_n, step, 0)

    def sum_copy(phase, move):
        peer = lax.rem(tp + move, tp_n)
        rows = pl.ds(aligned(peer * chunk, 16), chunk)
        return pltpu.make_async_remote_copy(
            src_ref=parts.at[phase, rows, :],
            dst_ref=landed.at[phase, move - 1],
            send_sem=sum_send.at[phase, move - 1],
            recv_sem=sum_recv.at[phase, move - 1],
            device_id={"tp": peer},
            device_id_type=MESH,
        )

    def put_copy(phase, move):
        rows = pl.ds(aligned(tp * chunk, 16), chunk)
        return pltpu.make_async_remote_copy(
            src_ref=streams.at[phase, rows, :],
            dst_ref=streams.at[phase, rows, :],
            send_sem=put_send.at[phase, move - 1],
            recv_sem=put_recv.at[phase, move - 1],
            device_id={"tp": lax.rem(tp + move, tp_n)},
            device_id_type=MESH,
        )

    def gain(row):
        return gains[row : row + 1, :].astype(F32)

    def norm_rows(load, row):
        def body(low):
            values = load(pl.ds(low, 32)).astype(F32)
            scale = lax.rsqrt(jnp.mean(values * values, axis=-1, keepdims=True) + 1e-06)
            normed[pl.ds(low, 32), :] = (values * scale * gain(row)).astype(BF16)

        over_rows(count, 32, body)

    def start_sums(phase):
        for move in range(1, tp_n):
            sum_copy(phase, move).start()

    def add_branch(phase, load, row, factor):
        for move in range(1, tp_n):
            sum_copy(phase, move).wait_recv()

        def body(low):
            rows = pl.ds(aligned(tp * chunk + low, 16), 16)
            total = parts[phase, rows, :].astype(F32)
            for move in range(1, tp_n):
                total = total + landed[phase, move - 1, pl.ds(low, 16), :].astype(F32)
            scale = lax.rsqrt(jnp.mean(total * total, axis=-1, keepdims=True) + 1e-06)
            branch = total * scale * gain(row)
            streams[phase, rows, :] = (load(rows).astype(F32) + factor * branch).astype(BF16)

        over_rows(chunk, 16, body)
        for move in range(1, tp_n):
            put_copy(phase, move).start()

    def wait_put(phase):
        for move in range(1, tp_n):
            put_copy(phase, move).wait_recv()

    def hidden_units():
        def body(low, size):
            cols = pl.ds(low, size)
            gate = jnp.dot(normed[...], gate_full[:, cols], preferred_element_type=F32)
            upper = jnp.dot(normed[...], up_full[:, cols], preferred_element_type=F32)
            hidden[:, cols] = (gate / (1.0 + jnp.exp(-gate)) * upper).astype(BF16)

        over_tiles(hidden.shape[1], body)

    def project(phase, left, right):
        size = right.shape[2]

        def one(block, low):
            terms = jnp.dot(left[...], right[block], preferred_element_type=F32)
            parts[phase, :, pl.ds(low, size)] = terms.astype(BF16)

        if size % 128 == 0:

            def step(block, carry):
                one(block, pl.multiple_of(block * size, 128))
                return carry

            lax.fori_loop(0, fs_n, step, 0)
        else:
            for block in range(fs_n):
                one(block, block * size)

    def mix():
        rows = lax.broadcasted_iota(jnp.int32, (BLOCK, BLOCK), 0)
        cols = lax.broadcasted_iota(jnp.int32, (BLOCK, BLOCK), 1)
        for g in range(mixed.shape[1] // GROUP_WIDTH):
            span = slice(g * GROUP_WIDTH, (g + 1) * GROUP_WIDTH)
            v = gelu(jnp.dot(normed[...], v_full[:, span], preferred_element_type=F32))
            u = gelu(jnp.dot(normed[...], u_full[:, span], preferred_element_type=F32))
            v = v - jnp.mean(v, axis=-1, keepdims=True)
            v = v * lax.rsqrt(jnp.mean(v * v, axis=-1, keepdims=True) + 1e-05)
            v = (v * spatial_gain[:, span].astype(F32)).astype(BF16)
            weight = spatial_weight[g].astype(F32)
            weight = jnp.where(rows >= cols, weight, 0.0).astype(BF16)
            for n in range(count // BLOCK):
                part = slice(n * BLOCK, (n + 1) * BLOCK)
                spatial = jnp.dot(weight, v[part], preferred_element_type=F32)
                spatial = spatial + spatial_bias[:, g : g + 1]
                mixed[part, span] = (u[part] * spatial).astype(BF16)

    load_tokens = lambda rows: tokens[rows, :]
    load_first = lambda rows: streams[0, rows, :]
    load_second = lambda rows: streams[1, rows, :]

    send_own(0)
    send_own(1)
    for w in range(6):
        own_copy(w).start()
    norm_rows(load_tokens, 0)

    def relay_weight(w):
        for unit in range(len(units)):
            if units[unit][0] == w:
                relay(unit)
                send_own(unit + 2)

    relay_weight(0)
    relay_weight(1)
    wait_weight(0)
    relay_weight(2)
    wait_weight(1)
    hidden_units()
    wait_weight(2)
    project(0, hidden, down_full)
    start_sums(0)
    relay_weight(3)
    add_branch(0, load_tokens, 1, 0.5)
    relay_weight(4)
    wait_put(0)
    norm_rows(load_first, 2)
    relay_weight(5)
    wait_weight(3)
    wait_weight(4)
    mix()
    wait_weight(5)
    project(1, mixed, out_full)
    start_sums(1)
    add_branch(1, load_first, 3, 1.0)
    wait_put(1)
    norm_rows(load_second, 4)
    hidden_units()
    project(2, hidden, down_full)
    start_sums(2)
    add_branch(2, load_second, 5, 0.5)
    finish_sends()
    wait_put(2)
    last = pltpu.make_async_copy(streams.at[2], result, last_sem)
    last.start()
    for phase in range(3):
        for move in range(1, tp_n):
            sum_copy(phase, move).wait_send()
            put_copy(phase, move).wait_send()
    last.wait()


def shards(
    sizes,
    tokens,
    ffn_pre_gain,
    gate_weight,
    up_weight,
    down_weight,
    ffn_post_gain,
    mix_pre_gain,
    mix_u_weight,
    mix_v_weight,
    spatial_gain,
    spatial_weight,
    spatial_bias,
    mix_out_weight,
    mix_post_gain,
    late_pre_gain,
    late_post_gain,
):
    grp_n, fs_n, tp_n = sizes
    count, width = tokens.shape
    hidden_width = gate_weight.shape[1]
    channels = mix_u_weight.shape[1]
    gains = jnp.stack(
        [ffn_pre_gain, ffn_post_gain, mix_pre_gain, mix_post_gain, late_pre_gain, late_post_gain]
    )
    vmem = pl.BlockSpec(memory_space=pltpu.VMEM)
    hbm = pl.BlockSpec(memory_space=pl.ANY)
    units = sum(SPLITS)
    dma = pltpu.SemaphoreType.DMA
    return pl.pallas_call(
        functools.partial(kernel, sizes),
        out_shape=jax.ShapeDtypeStruct((count, width), BF16),
        in_specs=[vmem, vmem, hbm, hbm, hbm, hbm, hbm, hbm, vmem, vmem, vmem],
        out_specs=hbm,
        scratch_shapes=[
            pltpu.VMEM((width, hidden_width), BF16),
            pltpu.VMEM((width, hidden_width), BF16),
            pltpu.VMEM((fs_n,) + down_weight.shape, BF16),
            pltpu.VMEM((width, channels), BF16),
            pltpu.VMEM((width, channels), BF16),
            pltpu.VMEM((fs_n,) + mix_out_weight.shape, BF16),
            pltpu.VMEM((count, width), BF16),
            pltpu.VMEM((count, hidden_width), BF16),
            pltpu.VMEM((count, channels), BF16),
            pltpu.VMEM((3, count, width), BF16),
            pltpu.VMEM((3, tp_n - 1, count // tp_n, width), BF16),
            pltpu.VMEM((3, count, width), BF16),
            dma((6,)),
            dma((units, fs_n)),
            dma((units, fs_n)),
            dma((units, fs_n)),
            dma((units, fs_n)),
            dma((units, 2, grp_n - 1, fs_n)),
            dma((units, 2, grp_n - 1, fs_n)),
            dma((3, tp_n - 1)),
            dma((3, tp_n - 1)),
            dma((3, tp_n - 1)),
            dma((3, tp_n - 1)),
            dma(()),
        ],
        compiler_params=pltpu.CompilerParams(
            collective_id=0, has_side_effects=True, vmem_limit_bytes=60 * 2**20
        ),
    )(
        tokens,
        gains,
        gate_weight,
        up_weight,
        down_weight,
        mix_u_weight,
        mix_v_weight,
        mix_out_weight,
        spatial_gain.reshape(1, channels),
        spatial_weight,
        spatial_bias.astype(F32).T,
    )


def solution(mesh):
    in_specs = (
        P(("grp", "fs"), None),
        P(),
        P("fs", "tp"),
        P("fs", "tp"),
        P("tp", "fs"),
        P(),
        P(),
        P("fs", "tp"),
        P("fs", "tp"),
        P("tp"),
        P("tp", None, None),
        P("tp", None),
        P("tp", "fs"),
        P(),
        P(),
        P(),
    )
    out_specs = P(("grp", "fs"), None)
    sizes = (mesh.shape["grp"], mesh.shape["fs"], mesh.shape["tp"])
    body = functools.partial(shards, sizes)
    return jax.shard_map(body, mesh=mesh, in_specs=in_specs, out_specs=out_specs, check_vma=False)
```

```python
import functools
import math

import jax
import jax.numpy as jnp
from jax import lax
from jax.experimental import pallas as pl
from jax.experimental.pallas import tpu as pltpu
from jax.sharding import PartitionSpec as P

GROUP_WIDTH = 128
BLOCK = 128
TILE = 256
F32 = jnp.float32
BF16 = jnp.bfloat16
MESH = pl.DeviceIdType.MESH
SPLITS = (2, 2, 2, 1, 1, 2)
PIECE = 32


def aligned(value, unit):
    return value if isinstance(value, int) else pl.multiple_of(value, unit)


def over_tiles(width, body):
    count = width // TILE

    def step(i, carry):
        body(pl.multiple_of(i * TILE, TILE), TILE)
        return carry

    lax.fori_loop(0, count, step, 0)
    if width % TILE:
        body(count * TILE, width % TILE)


def over_rows(count, size, body):
    def step(i, carry):
        body(pl.multiple_of(i * size, size))
        return carry

    lax.fori_loop(0, count // size, step, 0)


def gelu(a):
    return 0.5 * a * (1.0 + lax.erf(a * (2.0**-0.5)))


def kernel(
    sizes,
    tokens,
    gain0,
    gain1,
    gain2,
    gain3,
    gain4,
    gain5,
    gate_w,
    up_w,
    down_w,
    u_w,
    v_w,
    out_w,
    spatial_gain,
    spatial_weight,
    spatial_bias,
    result,
    gate_full,
    up_full,
    down_full,
    u_full,
    v_full,
    out_full,
    normed,
    hidden,
    mixed,
    parts,
    paired,
    outgoing,
    landed,
    streams,
    own_sem,
    left_send,
    left_recv,
    right_send,
    right_recv,
    side_send,
    side_recv,
    pair_send,
    pair_recv,
    sum_send,
    sum_recv,
    twin_send,
    twin_recv,
    put_send,
    put_recv,
    pass_send,
    pass_recv,
    last_sem,
):
    grp_n, fs_n, tp_n = sizes
    grp, fs, tp = lax.axis_index("grp"), lax.axis_index("fs"), lax.axis_index("tp")
    shards = (gate_w, up_w, down_w, u_w, v_w, out_w)
    fulls = (gate_full, up_full, down_full, u_full, v_full, out_full)
    count, width = tokens.shape
    chunk = count // tp_n
    chips = tp_n // 2
    chip, core = tp // 2, lax.rem(tp, 2)
    twin = tp + 1 - 2 * core
    columns = pair_send.shape[1]
    column = width // columns
    piece_n = put_send.shape[1]
    piece_rows = chunk // piece_n
    all_gains = (gain0, gain1, gain2, gain3, gain4, gain5)

    barrier = pltpu.get_barrier_semaphore()
    for move in (1, fs_n - 1):
        pl.semaphore_signal(
            barrier, inc=1, device_id={"fs": lax.rem(fs + move, fs_n)}, device_id_type=MESH
        )
    for move in range(1, grp_n):
        pl.semaphore_signal(
            barrier, inc=1, device_id={"grp": lax.rem(grp + move, grp_n)}, device_id_type=MESH
        )
    for move in range(1, tp_n):
        pl.semaphore_signal(
            barrier, inc=1, device_id={"tp": lax.rem(tp + move, tp_n)}, device_id_type=MESH
        )
    pl.semaphore_wait(barrier, 2 + grp_n - 1 + tp_n - 1)

    units = []
    for w in range(6):
        piece = shards[w].shape[0] // grp_n // SPLITS[w]
        for s in range(SPLITS[w]):
            units.append((w, s * piece, piece))

    def unit_rows(unit):
        w, low, piece = units[unit]
        return aligned(grp * (shards[w].shape[0] // grp_n) + low, 16), piece

    def place(w, block, low, piece):
        if w in (2, 5):
            return fulls[w].at[block, pl.ds(low, piece), :]
        start = aligned(block * shards[w].shape[0] + low, 16)
        return fulls[w].at[pl.ds(start, piece), :]

    def own_copy(w):
        return pltpu.make_async_copy(
            shards[w], place(w, fs, 0, shards[w].shape[0]), own_sem.at[w]
        )

    def to_right(unit, hop, own=False):
        w = units[unit][0]
        low, piece = unit_rows(unit)
        target = place(w, fs - hop, low, piece)
        source = shards[w].at[pl.ds(low, piece), :] if own else target
        return pltpu.make_async_remote_copy(
            src_ref=source,
            dst_ref=target,
            send_sem=right_send.at[unit, hop],
            recv_sem=right_recv.at[unit, hop],
            device_id={"fs": fs + 1},
            device_id_type=MESH,
        )

    def to_left(unit, hop, own=False):
        w = units[unit][0]
        low, piece = unit_rows(unit)
        target = place(w, fs + hop, low, piece)
        source = shards[w].at[pl.ds(low, piece), :] if own else target
        return pltpu.make_async_remote_copy(
            src_ref=source,
            dst_ref=target,
            send_sem=left_send.at[unit, hop],
            recv_sem=left_recv.at[unit, hop],
            device_id={"fs": fs - 1},
            device_id_type=MESH,
        )

    def to_side(unit, side, hop, move):
        w = units[unit][0]
        low, piece = unit_rows(unit)
        block = fs - hop if side == 0 else fs + hop
        target = place(w, block, low, piece)
        return pltpu.make_async_remote_copy(
            src_ref=target,
            dst_ref=target,
            send_sem=side_send.at[unit, side, move - 1, hop],
            recv_sem=side_recv.at[unit, side, move - 1, hop],
            device_id={"grp": lax.rem(grp + move, grp_n)},
            device_id_type=MESH,
        )

    def send_own(unit):
        if unit >= len(units):
            return

        @pl.when(fs < fs_n - 1)
        def _():
            to_right(unit, 0, own=True).start()

        @pl.when(fs > 0)
        def _():
            to_left(unit, 0, own=True).start()

    def relay(unit):
        def step(hop, carry):
            @pl.when(fs >= hop)
            def _():
                to_right(unit, hop - 1).wait_recv()

                @pl.when(fs < fs_n - 1)
                def _():
                    to_right(unit, hop).start()

                for move in range(1, grp_n):
                    to_side(unit, 0, hop, move).start()

            @pl.when(fs + hop < fs_n)
            def _():
                to_left(unit, hop - 1).wait_recv()

                @pl.when(fs > 0)
                def _():
                    to_left(unit, hop).start()

                for move in range(1, grp_n):
                    to_side(unit, 1, hop, move).start()

            return carry

        lax.fori_loop(1, fs_n, step, 0)

    def wait_weight(w):
        own_copy(w).wait()
        for unit in range(len(units)):
            if units[unit][0] == w:

                def step(hop, carry, unit=unit):
                    for move in range(1, grp_n):

                        @pl.when(fs >= hop)
                        def _():
                            to_side(unit, 0, hop, move).wait_recv()

                        @pl.when(fs + hop < fs_n)
                        def _():
                            to_side(unit, 1, hop, move).wait_recv()

                    return carry

                lax.fori_loop(1, fs_n, step, 0)

    def finish_sends():
        for unit in range(len(units)):

            def step(hop, carry, unit=unit):
                @pl.when((fs >= hop) & (fs < fs_n - 1))
                def _():
                    to_right(unit, hop).wait_send()

                @pl.when((fs + hop < fs_n) & (fs > 0))
                def _():
                    to_left(unit, hop).wait_send()

                @pl.when(hop > 0)
                def _():
                    for move in range(1, grp_n):

                        @pl.when(fs >= hop)
                        def _():
                            to_side(unit, 0, hop, move).wait_send()

                        @pl.when(fs + hop < fs_n)
                        def _():
                            to_side(unit, 1, hop, move).wait_send()

                return carry

            lax.fori_loop(0, fs_n, step, 0)

    def other(move, which):
        return lax.rem(chip + move, chips) * 2 + which

    def origin(move, which):
        return lax.rem(chip + chips - move, chips) * 2 + which

    def chunk_rows(owner):
        return pl.ds(aligned(owner * chunk, 16), chunk)

    def column_span(col):
        return pl.ds(aligned(col * column, 128), column)

    def pair_copy(phase, col, move):
        span = column_span(col)
        return pltpu.make_async_remote_copy(
            src_ref=parts.at[phase, chunk_rows(other(move, 1 - core)), span],
            dst_ref=paired.at[phase, move, :, span],
            send_sem=pair_send.at[phase, col, move],
            recv_sem=pair_recv.at[phase, col, move],
            device_id={"tp": twin},
            device_id_type=MESH,
        )

    def sum_copy(phase, col, move):
        span = column_span(col)
        return pltpu.make_async_remote_copy(
            src_ref=outgoing.at[phase, move, :, span],
            dst_ref=landed.at[phase, move, :, span],
            send_sem=sum_send.at[phase, col, move],
            recv_sem=sum_recv.at[phase, col, move],
            device_id={"tp": other(move, core)},
            device_id_type=MESH,
        )

    def piece_span(owner, piece):
        return pl.ds(aligned(owner * chunk + piece * piece_rows, 16), piece_rows)

    def twin_copy(phase, piece):
        rows = piece_span(tp, piece)
        return pltpu.make_async_remote_copy(
            src_ref=streams.at[phase, rows, :],
            dst_ref=streams.at[phase, rows, :],
            send_sem=twin_send.at[phase, piece],
            recv_sem=twin_recv.at[phase, piece],
            device_id={"tp": twin},
            device_id_type=MESH,
        )

    def put_copy(phase, piece, move):
        rows = piece_span(tp, piece)
        return pltpu.make_async_remote_copy(
            src_ref=streams.at[phase, rows, :],
            dst_ref=streams.at[phase, rows, :],
            send_sem=put_send.at[phase, piece, move],
            recv_sem=put_recv.at[phase, piece, move],
            device_id={"tp": other(move, core)},
            device_id_type=MESH,
        )

    def pass_copy(phase, piece, move):
        rows = piece_span(origin(move, core), piece)
        return pltpu.make_async_remote_copy(
            src_ref=streams.at[phase, rows, :],
            dst_ref=streams.at[phase, rows, :],
            send_sem=pass_send.at[phase, piece, move],
            recv_sem=pass_recv.at[phase, piece, move],
            device_id={"tp": twin},
            device_id_type=MESH,
        )

    def gain(row):
        return all_gains[row][...].astype(F32).reshape(1, width)

    def norm_rows(load, row):
        def body(low):
            values = load(pl.ds(low, 32)).astype(F32)
            scale = lax.rsqrt(jnp.mean(values * values, axis=-1, keepdims=True) + 1e-06)
            normed[pl.ds(low, 32), :] = (values * scale * gain(row)).astype(BF16)

        over_rows(count, 32, body)

    def start_sums(phase, col):
        for move in range(1, chips):
            pair_copy(phase, col, move).wait_recv()
            span = column_span(col)
            mine = parts[phase, chunk_rows(other(move, core)), span].astype(F32)
            both = mine + paired[phase, move, :, span].astype(F32)
            outgoing[phase, move, :, span] = both.astype(BF16)
            sum_copy(phase, col, move).start()

    def add_branch(phase, load, row, factor):
        for col in range(columns):
            pair_copy(phase, col, 0).wait_recv()
            for move in range(1, chips):
                sum_copy(phase, col, move).wait_recv()
        for piece in range(piece_n):

            def body(low, piece=piece):
                here = pl.ds(aligned(piece * piece_rows + low, 16), 16)
                rows = pl.ds(aligned(tp * chunk + piece * piece_rows + low, 16), 16)
                total = parts[phase, rows, :].astype(F32) + paired[phase, 0, here, :].astype(F32)
                for move in range(1, chips):
                    total = total + landed[phase, move, here, :].astype(F32)
                scale = lax.rsqrt(jnp.mean(total * total, axis=-1, keepdims=True) + 1e-06)
                branch = total * scale * gain(row)
                streams[phase, rows, :] = (load(rows).astype(F32) + factor * branch).astype(BF16)

            over_rows(piece_rows, 16, body)
            for move in range(1, chips):
                put_copy(phase, piece, move).start()
            twin_copy(phase, piece).start()

    def wait_put(phase):
        for piece in range(piece_n):
            for move in range(1, chips):
                put_copy(phase, piece, move).wait_recv()
                pass_copy(phase, piece, move).start()
        for piece in range(piece_n):
            twin_copy(phase, piece).wait_recv()
            for move in range(1, chips):
                pass_copy(phase, piece, move).wait_recv()

    def finish_phase(phase):
        for col in range(columns):
            for move in range(chips):
                pair_copy(phase, col, move).wait_send()
            for move in range(1, chips):
                sum_copy(phase, col, move).wait_send()
        for piece in range(piece_n):
            twin_copy(phase, piece).wait_send()
            for move in range(1, chips):
                put_copy(phase, piece, move).wait_send()
                pass_copy(phase, piece, move).wait_send()

    def hidden_units():
        def body(low, size):
            cols = pl.ds(low, size)
            gate = jnp.dot(normed[...], gate_full[:, cols], preferred_element_type=F32)
            upper = jnp.dot(normed[...], up_full[:, cols], preferred_element_type=F32)
            hidden[:, cols] = (gate / (1.0 + jnp.exp(-gate)) * upper).astype(BF16)

        over_tiles(hidden.shape[1], body)

    def project(phase, left, right):
        blocks = fs_n // columns

        def step(col, carry):
            terms = [
                jnp.dot(left[...], right[col * blocks + b], preferred_element_type=F32)
                for b in range(blocks)
            ]
            terms = terms[0] if blocks == 1 else jnp.concatenate(terms, axis=1)
            parts[phase, :, column_span(col)] = terms.astype(BF16)
            for move in range(chips - 1, -1, -1):
                pair_copy(phase, col, move).start()

            @pl.when(col > 0)
            def _():
                start_sums(phase, col - 1)

            return carry

        lax.fori_loop(0, columns, step, 0)
        start_sums(phase, columns - 1)

    def mix():
        rows = lax.broadcasted_iota(jnp.int32, (BLOCK, BLOCK), 0)
        cols = lax.broadcasted_iota(jnp.int32, (BLOCK, BLOCK), 1)
        all_spatial_gain = spatial_gain[...].astype(F32).reshape(1, mixed.shape[1])
        for g in range(mixed.shape[1] // GROUP_WIDTH):
            span = slice(g * GROUP_WIDTH, (g + 1) * GROUP_WIDTH)
            v = gelu(jnp.dot(normed[...], v_full[:, span], preferred_element_type=F32))
            u = gelu(jnp.dot(normed[...], u_full[:, span], preferred_element_type=F32))
            v = v - jnp.mean(v, axis=-1, keepdims=True)
            v = v * lax.rsqrt(jnp.mean(v * v, axis=-1, keepdims=True) + 1e-05)
            v = (v * all_spatial_gain[:, span]).astype(BF16)
            weight = spatial_weight[g].astype(F32)
            weight = jnp.where(rows >= cols, weight, 0.0).astype(BF16)
            bias = spatial_bias[...][g : g + 1, :].astype(F32)
            bias = jnp.sum(jnp.where(rows == cols, bias, 0.0), axis=1, keepdims=True)
            for n in range(count // BLOCK):
                part = slice(n * BLOCK, (n + 1) * BLOCK)
                spatial = jnp.dot(weight, v[part], preferred_element_type=F32)
                spatial = spatial + bias
                mixed[part, span] = (u[part] * spatial).astype(BF16)

    load_tokens = lambda rows: tokens[rows, :]
    load_first = lambda rows: streams[0, rows, :]
    load_second = lambda rows: streams[1, rows, :]

    send_own(0)
    send_own(1)
    for w in range(6):
        own_copy(w).start()
    norm_rows(load_tokens, 0)

    for unit in range(5):
        relay(unit)
        send_own(unit + 2)
    wait_weight(0)
    wait_weight(1)
    hidden_units()
    relay(5)
    send_own(7)
    relay(6)
    send_own(8)
    send_own(9)
    wait_weight(2)
    project(0, hidden, down_full)
    relay(7)
    add_branch(0, load_tokens, 1, 0.5)
    relay(8)
    wait_put(0)
    norm_rows(load_first, 2)
    relay(9)
    wait_weight(3)
    wait_weight(4)
    mix()
    wait_weight(5)
    project(1, mixed, out_full)
    add_branch(1, load_first, 3, 1.0)
    wait_put(1)
    norm_rows(load_second, 4)
    hidden_units()
    project(2, hidden, down_full)
    add_branch(2, load_second, 5, 0.5)
    finish_sends()
    wait_put(2)
    last = pltpu.make_async_copy(streams.at[2], result, last_sem)
    last.start()
    for phase in range(3):
        finish_phase(phase)
    last.wait()


def shards(
    sizes,
    tokens,
    ffn_pre_gain,
    gate_weight,
    up_weight,
    down_weight,
    ffn_post_gain,
    mix_pre_gain,
    mix_u_weight,
    mix_v_weight,
    spatial_gain,
    spatial_weight,
    spatial_bias,
    mix_out_weight,
    mix_post_gain,
    late_pre_gain,
    late_post_gain,
):
    grp_n, fs_n, tp_n = sizes
    count, width = tokens.shape
    hidden_width = gate_weight.shape[1]
    channels = mix_u_weight.shape[1]
    columns = math.gcd(fs_n, 4)
    chips = tp_n // 2
    chunk = count // tp_n
    pieces = max(1, chunk // PIECE)
    vmem = pl.BlockSpec(memory_space=pltpu.VMEM)
    hbm = pl.BlockSpec(memory_space=pl.ANY)
    units = sum(SPLITS)
    dma = pltpu.SemaphoreType.DMA
    return pl.pallas_call(
        functools.partial(kernel, sizes),
        out_shape=jax.ShapeDtypeStruct((count, width), BF16),
        in_specs=[vmem] * 7 + [hbm, hbm, hbm, hbm, hbm, hbm, vmem, vmem, vmem],
        out_specs=hbm,
        scratch_shapes=[
            pltpu.VMEM((width, hidden_width), BF16),
            pltpu.VMEM((width, hidden_width), BF16),
            pltpu.VMEM((fs_n,) + down_weight.shape, BF16),
            pltpu.VMEM((width, channels), BF16),
            pltpu.VMEM((width, channels), BF16),
            pltpu.VMEM((fs_n,) + mix_out_weight.shape, BF16),
            pltpu.VMEM((count, width), BF16),
            pltpu.VMEM((count, hidden_width), BF16),
            pltpu.VMEM((count, channels), BF16),
            pltpu.VMEM((3, count, width), BF16),
            pltpu.VMEM((3, chips, chunk, width), BF16),
            pltpu.VMEM((3, chips, chunk, width), BF16),
            pltpu.VMEM((3, chips, chunk, width), BF16),
            pltpu.VMEM((3, count, width), BF16),
            dma((6,)),
            dma((units, fs_n)),
            dma((units, fs_n)),
            dma((units, fs_n)),
            dma((units, fs_n)),
            dma((units, 2, grp_n - 1, fs_n)),
            dma((units, 2, grp_n - 1, fs_n)),
            dma((3, columns, chips)),
            dma((3, columns, chips)),
            dma((3, columns, chips)),
            dma((3, columns, chips)),
            dma((3, pieces)),
            dma((3, pieces)),
            dma((3, pieces, chips)),
            dma((3, pieces, chips)),
            dma((3, pieces, chips)),
            dma((3, pieces, chips)),
            dma(()),
        ],
        compiler_params=pltpu.CompilerParams(
            collective_id=0, has_side_effects=True, vmem_limit_bytes=60 * 2**20
        ),
    )(
        tokens,
        ffn_pre_gain,
        ffn_post_gain,
        mix_pre_gain,
        mix_post_gain,
        late_pre_gain,
        late_post_gain,
        gate_weight,
        up_weight,
        down_weight,
        mix_u_weight,
        mix_v_weight,
        mix_out_weight,
        spatial_gain,
        spatial_weight,
        spatial_bias,
    )


def solution(mesh):
    in_specs = (
        P(("grp", "fs"), None),
        P(),
        P("fs", "tp"),
        P("fs", "tp"),
        P("tp", "fs"),
        P(),
        P(),
        P("fs", "tp"),
        P("fs", "tp"),
        P("tp"),
        P("tp", None, None),
        P("tp", None),
        P("tp", "fs"),
        P(),
        P(),
        P(),
    )
    out_specs = P(("grp", "fs"), None)
    sizes = (mesh.shape["grp"], mesh.shape["fs"], mesh.shape["tp"])
    body = functools.partial(shards, sizes)
    return jax.shard_map(body, mesh=mesh, in_specs=in_specs, out_specs=out_specs, check_vma=False)
```

```python
import functools
import math

import jax
import jax.numpy as jnp
from jax import lax
from jax.experimental import pallas as pl
from jax.experimental.pallas import tpu as pltpu
from jax.sharding import PartitionSpec as P

GROUP_WIDTH = 128
BLOCK = 128
TILE = 256
F32 = jnp.float32
BF16 = jnp.bfloat16
MESH = pl.DeviceIdType.MESH
SPLITS = (2, 2, 2, 1, 1, 2)
PIECE = 32


def aligned(value, unit):
    return value if isinstance(value, int) else pl.multiple_of(value, unit)


def over_tiles(width, body, third, thirds):
    count = width // TILE

    def step(i, carry):
        body(pl.multiple_of(i * TILE, TILE), TILE)
        return carry

    lax.fori_loop(count * third // thirds, count * (third + 1) // thirds, step, 0)
    if width % TILE and third == thirds - 1:
        body(count * TILE, width % TILE)


def over_rows(count, size, body):
    def step(i, carry):
        body(pl.multiple_of(i * size, size))
        return carry

    lax.fori_loop(0, count // size, step, 0)


def gelu(a):
    return 0.5 * a * (1.0 + lax.erf(a * (2.0**-0.5)))


def kernel(
    sizes,
    tokens,
    gain0,
    gain1,
    gain2,
    gain3,
    gain4,
    gain5,
    gate_w,
    up_w,
    down_w,
    u_w,
    v_w,
    out_w,
    spatial_gain,
    spatial_weight,
    spatial_bias,
    result,
    gate_full,
    up_full,
    down_full,
    u_full,
    v_full,
    out_full,
    normed,
    hidden,
    mixed,
    parts,
    paired,
    outgoing,
    landed,
    streams,
    own_sem,
    left_send,
    left_recv,
    right_send,
    right_recv,
    side_send,
    side_recv,
    pair_send,
    pair_recv,
    sum_send,
    sum_recv,
    twin_send,
    twin_recv,
    put_send,
    put_recv,
    pass_send,
    pass_recv,
    last_sem,
):
    grp_n, fs_n, tp_n = sizes
    grp, fs, tp = lax.axis_index("grp"), lax.axis_index("fs"), lax.axis_index("tp")
    shards = (gate_w, up_w, down_w, u_w, v_w, out_w)
    fulls = (gate_full, up_full, down_full, u_full, v_full, out_full)
    count, width = tokens.shape
    chunk = count // tp_n
    chips = tp_n // 2
    chip, core = tp // 2, lax.rem(tp, 2)
    twin = tp + 1 - 2 * core
    columns = pair_send.shape[1]
    column = width // columns
    piece_n = put_send.shape[1]
    piece_rows = chunk // piece_n
    all_gains = (gain0, gain1, gain2, gain3, gain4, gain5)

    barrier = pltpu.get_barrier_semaphore()
    for move in (1, fs_n - 1):
        pl.semaphore_signal(
            barrier, inc=1, device_id={"fs": lax.rem(fs + move, fs_n)}, device_id_type=MESH
        )
    for move in range(1, grp_n):
        pl.semaphore_signal(
            barrier, inc=1, device_id={"grp": lax.rem(grp + move, grp_n)}, device_id_type=MESH
        )
    for move in range(1, tp_n):
        pl.semaphore_signal(
            barrier, inc=1, device_id={"tp": lax.rem(tp + move, tp_n)}, device_id_type=MESH
        )
    pl.semaphore_wait(barrier, 2 + grp_n - 1 + tp_n - 1)

    units = []
    for w in range(6):
        piece = shards[w].shape[0] // grp_n // SPLITS[w]
        for s in range(SPLITS[w]):
            units.append((w, s * piece, piece))

    def unit_rows(unit):
        w, low, piece = units[unit]
        return aligned(grp * (shards[w].shape[0] // grp_n) + low, 16), piece

    def place(w, block, low, piece):
        if w in (2, 5):
            return fulls[w].at[block, pl.ds(low, piece), :]
        start = aligned(block * shards[w].shape[0] + low, 16)
        return fulls[w].at[pl.ds(start, piece), :]

    def own_copy(w):
        return pltpu.make_async_copy(
            shards[w], place(w, fs, 0, shards[w].shape[0]), own_sem.at[w]
        )

    def to_right(unit, hop, own=False):
        w = units[unit][0]
        low, piece = unit_rows(unit)
        target = place(w, fs - hop, low, piece)
        source = shards[w].at[pl.ds(low, piece), :] if own else target
        return pltpu.make_async_remote_copy(
            src_ref=source,
            dst_ref=target,
            send_sem=right_send.at[unit, hop],
            recv_sem=right_recv.at[unit, hop],
            device_id={"fs": fs + 1},
            device_id_type=MESH,
        )

    def to_left(unit, hop, own=False):
        w = units[unit][0]
        low, piece = unit_rows(unit)
        target = place(w, fs + hop, low, piece)
        source = shards[w].at[pl.ds(low, piece), :] if own else target
        return pltpu.make_async_remote_copy(
            src_ref=source,
            dst_ref=target,
            send_sem=left_send.at[unit, hop],
            recv_sem=left_recv.at[unit, hop],
            device_id={"fs": fs - 1},
            device_id_type=MESH,
        )

    def to_side(unit, side, hop, move):
        w = units[unit][0]
        low, piece = unit_rows(unit)
        block = fs - hop if side == 0 else fs + hop
        target = place(w, block, low, piece)
        return pltpu.make_async_remote_copy(
            src_ref=target,
            dst_ref=target,
            send_sem=side_send.at[unit, side, move - 1, hop],
            recv_sem=side_recv.at[unit, side, move - 1, hop],
            device_id={"grp": lax.rem(grp + move, grp_n)},
            device_id_type=MESH,
        )

    def send_own(unit):
        if unit >= len(units):
            return

        @pl.when(fs < fs_n - 1)
        def _():
            to_right(unit, 0, own=True).start()

        @pl.when(fs > 0)
        def _():
            to_left(unit, 0, own=True).start()

    def relay(unit, low=1, high=fs_n):
        def step(hop, carry):
            @pl.when(fs >= hop)
            def _():
                to_right(unit, hop - 1).wait_recv()

                @pl.when(fs < fs_n - 1)
                def _():
                    to_right(unit, hop).start()

                for move in range(1, grp_n):
                    to_side(unit, 0, hop, move).start()

            @pl.when(fs + hop < fs_n)
            def _():
                to_left(unit, hop - 1).wait_recv()

                @pl.when(fs > 0)
                def _():
                    to_left(unit, hop).start()

                for move in range(1, grp_n):
                    to_side(unit, 1, hop, move).start()

            return carry

        lax.fori_loop(low, high, step, 0)

    def wait_weight(w):
        own_copy(w).wait()
        for unit in range(len(units)):
            if units[unit][0] == w:

                def step(hop, carry, unit=unit):
                    for move in range(1, grp_n):

                        @pl.when(fs >= hop)
                        def _():
                            to_side(unit, 0, hop, move).wait_recv()

                        @pl.when(fs + hop < fs_n)
                        def _():
                            to_side(unit, 1, hop, move).wait_recv()

                    return carry

                lax.fori_loop(1, fs_n, step, 0)

    def finish_sends():
        for unit in range(len(units)):

            def step(hop, carry, unit=unit):
                @pl.when((fs >= hop) & (fs < fs_n - 1))
                def _():
                    to_right(unit, hop).wait_send()

                @pl.when((fs + hop < fs_n) & (fs > 0))
                def _():
                    to_left(unit, hop).wait_send()

                @pl.when(hop > 0)
                def _():
                    for move in range(1, grp_n):

                        @pl.when(fs >= hop)
                        def _():
                            to_side(unit, 0, hop, move).wait_send()

                        @pl.when(fs + hop < fs_n)
                        def _():
                            to_side(unit, 1, hop, move).wait_send()

                return carry

            lax.fori_loop(0, fs_n, step, 0)

    def other(move, which):
        return lax.rem(chip + move, chips) * 2 + which

    def origin(move, which):
        return lax.rem(chip + chips - move, chips) * 2 + which

    def chunk_rows(owner):
        return pl.ds(aligned(owner * chunk, 16), chunk)

    def column_span(col):
        return pl.ds(aligned(col * column, 128), column)

    def pair_copy(phase, col, move):
        span = column_span(col)
        return pltpu.make_async_remote_copy(
            src_ref=parts.at[phase, chunk_rows(other(move, 1 - core)), span],
            dst_ref=paired.at[phase, move, :, span],
            send_sem=pair_send.at[phase, col, move],
            recv_sem=pair_recv.at[phase, col, move],
            device_id={"tp": twin},
            device_id_type=MESH,
        )

    def sum_copy(phase, col, move):
        span = column_span(col)
        return pltpu.make_async_remote_copy(
            src_ref=outgoing.at[phase, move, :, span],
            dst_ref=landed.at[phase, move, :, span],
            send_sem=sum_send.at[phase, col, move],
            recv_sem=sum_recv.at[phase, col, move],
            device_id={"tp": other(move, core)},
            device_id_type=MESH,
        )

    def piece_span(owner, piece):
        return pl.ds(aligned(owner * chunk + piece * piece_rows, 16), piece_rows)

    def twin_copy(phase, piece):
        rows = piece_span(tp, piece)
        return pltpu.make_async_remote_copy(
            src_ref=streams.at[phase, rows, :],
            dst_ref=streams.at[phase, rows, :],
            send_sem=twin_send.at[phase, piece],
            recv_sem=twin_recv.at[phase, piece],
            device_id={"tp": twin},
            device_id_type=MESH,
        )

    def put_copy(phase, piece, move):
        rows = piece_span(tp, piece)
        return pltpu.make_async_remote_copy(
            src_ref=streams.at[phase, rows, :],
            dst_ref=streams.at[phase, rows, :],
            send_sem=put_send.at[phase, piece, move],
            recv_sem=put_recv.at[phase, piece, move],
            device_id={"tp": other(move, core)},
            device_id_type=MESH,
        )

    def pass_copy(phase, piece, move):
        rows = piece_span(origin(move, core), piece)
        return pltpu.make_async_remote_copy(
            src_ref=streams.at[phase, rows, :],
            dst_ref=streams.at[phase, rows, :],
            send_sem=pass_send.at[phase, piece, move],
            recv_sem=pass_recv.at[phase, piece, move],
            device_id={"tp": twin},
            device_id_type=MESH,
        )

    def gain(row):
        return all_gains[row][...].astype(F32).reshape(1, width)

    def norm_rows(load, row):
        def body(low):
            values = load(pl.ds(low, 32)).astype(F32)
            scale = lax.rsqrt(jnp.mean(values * values, axis=-1, keepdims=True) + 1e-06)
            normed[pl.ds(low, 32), :] = (values * scale * gain(row)).astype(BF16)

        over_rows(count, 32, body)

    def start_sums(phase, col):
        for move in range(1, chips):
            pair_copy(phase, col, move).wait_recv()
            span = column_span(col)
            mine = parts[phase, chunk_rows(other(move, core)), span].astype(F32)
            both = mine + paired[phase, move, :, span].astype(F32)
            outgoing[phase, move, :, span] = both.astype(BF16)
            sum_copy(phase, col, move).start()

    def add_branch(phase, load, row, factor):
        for col in range(columns):
            pair_copy(phase, col, 0).wait_recv()
            for move in range(1, chips):
                sum_copy(phase, col, move).wait_recv()
        for piece in range(piece_n):

            def body(low, piece=piece):
                here = pl.ds(aligned(piece * piece_rows + low, 16), 16)
                rows = pl.ds(aligned(tp * chunk + piece * piece_rows + low, 16), 16)
                total = parts[phase, rows, :].astype(F32) + paired[phase, 0, here, :].astype(F32)
                for move in range(1, chips):
                    total = total + landed[phase, move, here, :].astype(F32)
                scale = lax.rsqrt(jnp.mean(total * total, axis=-1, keepdims=True) + 1e-06)
                branch = total * scale * gain(row)
                streams[phase, rows, :] = (load(rows).astype(F32) + factor * branch).astype(BF16)

            over_rows(piece_rows, 16, body)
            for move in range(1, chips):
                put_copy(phase, piece, move).start()
            twin_copy(phase, piece).start()

    def wait_put(phase):
        for piece in range(piece_n):
            for move in range(1, chips):
                put_copy(phase, piece, move).wait_recv()
                pass_copy(phase, piece, move).start()
        for piece in range(piece_n):
            twin_copy(phase, piece).wait_recv()
            for move in range(1, chips):
                pass_copy(phase, piece, move).wait_recv()

    def finish_phase(phase):
        for col in range(columns):
            for move in range(chips):
                pair_copy(phase, col, move).wait_send()
            for move in range(1, chips):
                sum_copy(phase, col, move).wait_send()
        for piece in range(piece_n):
            twin_copy(phase, piece).wait_send()
            for move in range(1, chips):
                put_copy(phase, piece, move).wait_send()
                pass_copy(phase, piece, move).wait_send()

    def hidden_units(third=0, thirds=1):
        def body(low, size):
            cols = pl.ds(low, size)
            gate = jnp.dot(normed[...], gate_full[:, cols], preferred_element_type=F32)
            upper = jnp.dot(normed[...], up_full[:, cols], preferred_element_type=F32)
            hidden[:, cols] = (gate / (1.0 + jnp.exp(-gate)) * upper).astype(BF16)

        over_tiles(hidden.shape[1], body, third, thirds)

    def project(phase, left, right):
        blocks = fs_n // columns

        def step(col, carry):
            terms = [
                jnp.dot(left[...], right[col * blocks + b], preferred_element_type=F32)
                for b in range(blocks)
            ]
            terms = terms[0] if blocks == 1 else jnp.concatenate(terms, axis=1)
            parts[phase, :, column_span(col)] = terms.astype(BF16)
            for move in range(chips - 1, -1, -1):
                pair_copy(phase, col, move).start()

            @pl.when(col > 0)
            def _():
                start_sums(phase, col - 1)

            return carry

        lax.fori_loop(0, columns, step, 0)
        start_sums(phase, columns - 1)

    def mix():
        rows = lax.broadcasted_iota(jnp.int32, (BLOCK, BLOCK), 0)
        cols = lax.broadcasted_iota(jnp.int32, (BLOCK, BLOCK), 1)
        all_spatial_gain = spatial_gain[...].astype(F32).reshape(1, mixed.shape[1])
        for g in range(mixed.shape[1] // GROUP_WIDTH):
            span = slice(g * GROUP_WIDTH, (g + 1) * GROUP_WIDTH)
            v = gelu(jnp.dot(normed[...], v_full[:, span], preferred_element_type=F32))
            u = gelu(jnp.dot(normed[...], u_full[:, span], preferred_element_type=F32))
            v = v - jnp.mean(v, axis=-1, keepdims=True)
            v = v * lax.rsqrt(jnp.mean(v * v, axis=-1, keepdims=True) + 1e-05)
            v = (v * all_spatial_gain[:, span]).astype(BF16)
            weight = spatial_weight[g].astype(F32)
            weight = jnp.where(rows >= cols, weight, 0.0).astype(BF16)
            bias = spatial_bias[...][g : g + 1, :].astype(F32)
            bias = jnp.sum(jnp.where(rows == cols, bias, 0.0), axis=1, keepdims=True)
            for n in range(count // BLOCK):
                part = slice(n * BLOCK, (n + 1) * BLOCK)
                spatial = jnp.dot(weight, v[part], preferred_element_type=F32)
                spatial = spatial + bias
                mixed[part, span] = (u[part] * spatial).astype(BF16)

    load_tokens = lambda rows: tokens[rows, :]
    load_first = lambda rows: streams[0, rows, :]
    load_second = lambda rows: streams[1, rows, :]

    send_own(0)
    send_own(1)
    for w in range(6):
        own_copy(w).start()
    norm_rows(load_tokens, 0)

    for unit in range(5):
        relay(unit)
        send_own(unit + 2)
    wait_weight(0)
    wait_weight(1)
    for third in range(3):
        hidden_units(third, 3)
        relay(5, min(1 + third, fs_n), fs_n if third == 2 else min(2 + third, fs_n))
    send_own(7)
    relay(6)
    send_own(8)
    send_own(9)
    wait_weight(2)
    project(0, hidden, down_full)
    relay(7)
    add_branch(0, load_tokens, 1, 0.5)
    relay(8)
    wait_put(0)
    norm_rows(load_first, 2)
    relay(9)
    wait_weight(3)
    wait_weight(4)
    mix()
    wait_weight(5)
    project(1, mixed, out_full)
    add_branch(1, load_first, 3, 1.0)
    wait_put(1)
    norm_rows(load_second, 4)
    hidden_units()
    project(2, hidden, down_full)
    add_branch(2, load_second, 5, 0.5)
    finish_sends()
    wait_put(2)
    last = pltpu.make_async_copy(streams.at[2], result, last_sem)
    last.start()
    for phase in range(3):
        finish_phase(phase)
    last.wait()


def shards(
    sizes,
    tokens,
    ffn_pre_gain,
    gate_weight,
    up_weight,
    down_weight,
    ffn_post_gain,
    mix_pre_gain,
    mix_u_weight,
    mix_v_weight,
    spatial_gain,
    spatial_weight,
    spatial_bias,
    mix_out_weight,
    mix_post_gain,
    late_pre_gain,
    late_post_gain,
):
    grp_n, fs_n, tp_n = sizes
    count, width = tokens.shape
    hidden_width = gate_weight.shape[1]
    channels = mix_u_weight.shape[1]
    columns = math.gcd(fs_n, 4)
    chips = tp_n // 2
    chunk = count // tp_n
    pieces = max(1, chunk // PIECE)
    vmem = pl.BlockSpec(memory_space=pltpu.VMEM)
    hbm = pl.BlockSpec(memory_space=pl.ANY)
    units = sum(SPLITS)
    dma = pltpu.SemaphoreType.DMA
    return pl.pallas_call(
        functools.partial(kernel, sizes),
        out_shape=jax.ShapeDtypeStruct((count, width), BF16),
        in_specs=[vmem] * 7 + [hbm, hbm, hbm, hbm, hbm, hbm, vmem, vmem, vmem],
        out_specs=hbm,
        scratch_shapes=[
            pltpu.VMEM((width, hidden_width), BF16),
            pltpu.VMEM((width, hidden_width), BF16),
            pltpu.VMEM((fs_n,) + down_weight.shape, BF16),
            pltpu.VMEM((width, channels), BF16),
            pltpu.VMEM((width, channels), BF16),
            pltpu.VMEM((fs_n,) + mix_out_weight.shape, BF16),
            pltpu.VMEM((count, width), BF16),
            pltpu.VMEM((count, hidden_width), BF16),
            pltpu.VMEM((count, channels), BF16),
            pltpu.VMEM((3, count, width), BF16),
            pltpu.VMEM((3, chips, chunk, width), BF16),
            pltpu.VMEM((3, chips, chunk, width), BF16),
            pltpu.VMEM((3, chips, chunk, width), BF16),
            pltpu.VMEM((3, count, width), BF16),
            dma((6,)),
            dma((units, fs_n)),
            dma((units, fs_n)),
            dma((units, fs_n)),
            dma((units, fs_n)),
            dma((units, 2, grp_n - 1, fs_n)),
            dma((units, 2, grp_n - 1, fs_n)),
            dma((3, columns, chips)),
            dma((3, columns, chips)),
            dma((3, columns, chips)),
            dma((3, columns, chips)),
            dma((3, pieces)),
            dma((3, pieces)),
            dma((3, pieces, chips)),
            dma((3, pieces, chips)),
            dma((3, pieces, chips)),
            dma((3, pieces, chips)),
            dma(()),
        ],
        compiler_params=pltpu.CompilerParams(
            collective_id=0, has_side_effects=True, vmem_limit_bytes=60 * 2**20
        ),
    )(
        tokens,
        ffn_pre_gain,
        ffn_post_gain,
        mix_pre_gain,
        mix_post_gain,
        late_pre_gain,
        late_post_gain,
        gate_weight,
        up_weight,
        down_weight,
        mix_u_weight,
        mix_v_weight,
        mix_out_weight,
        spatial_gain,
        spatial_weight,
        spatial_bias,
    )


def solution(mesh):
    in_specs = (
        P(("grp", "fs"), None),
        P(),
        P("fs", "tp"),
        P("fs", "tp"),
        P("tp", "fs"),
        P(),
        P(),
        P("fs", "tp"),
        P("fs", "tp"),
        P("tp"),
        P("tp", None, None),
        P("tp", None),
        P("tp", "fs"),
        P(),
        P(),
        P(),
    )
    out_specs = P(("grp", "fs"), None)
    sizes = (mesh.shape["grp"], mesh.shape["fs"], mesh.shape["tp"])
    body = functools.partial(shards, sizes)
    return jax.shard_map(body, mesh=mesh, in_specs=in_specs, out_specs=out_specs, check_vma=False)
```
